32 devices in a mesh: grp: 2 (over y), fs: 4 (over z), tp: 4 (over x, core).
Axes of the slice: x: 2, y: 2, z: 4, core: 2. Of those that a mesh axis runs over, the one named last changes fastest.
Arguments:
- tokens: bfloat16 [1536, 2048], P(('grp', 'tp')), parts along dimension 0, may hold values from -6 to 6
- routes: int32 [1536, 2], P(('grp', 'tp')), parts along dimension 0, may hold values from 0 to 3, all different within a row; in each aligned block of 192 rows (0 to 191, 192 to 383, ...) at most 128 rows name the same one
- route_weight: float32 [1536, 2], P(('grp', 'tp')), parts along dimension 0, may hold values from 0.2 to 1
- norm_gain: float32 [2048], P('fs'), may hold values from 0.1 to 1.9
- gate_train: float32 [4, 2048, 5632], P('tp', 'fs'), may hold values from -0.125 to 0.125
- up_train: float32 [4, 2048, 5632], P('tp', 'fs'), may hold values from -0.125 to 0.125
- down_train: float32 [4, 5632, 2048], P('tp', None, 'fs'), may hold values from -0.109375 to 0.109375
Outputs:
- gate_serve: bfloat16 [8, 2048, 5632], P(('grp', 'tp'), None, 'fs'), parts along dimension 0
- up_serve: bfloat16 [8, 2048, 5632], P(('grp', 'tp'), None, 'fs'), parts along dimension 0
- down_serve: bfloat16 [8, 5632, 2048], P(('grp', 'tp'), 'fs'), parts along dimension 0
- mixed: bfloat16 [1536, 2048], P(('grp', 'tp'), 'fs'), parts along dimension 0
The draws below stay inside these ranges and needn't reach their ends.
There are 2 independent parts, one for each index of `grp`. The reference program is written for one: setup_inputs(seed, part) draws one part's arguments, and reference() takes and returns one part's arrays. A program takes and returns all parts, laid end to end along the dimension named above; an argument that names none is the same for every part. Nothing has to cross between parts.
Inputs may be any that keep to these rules, and one draw needn't show every extreme that they name: `routes`: each row names 2 different experts. In each aligned block of 192 rows no expert is named by more than 128 rows, a bound that some block reaches.
All inputs are finite; a program needn't handle non-finite values.
Results may differ from the reference program's by a relative error of at most 0.0087.
Values may be sent and summed in bfloat16 or wider, within the bound.
No kernel may reach another device: no remote copies, remote signals or barrier semaphores. Data moves between devices by JAX's collectives and lax.ppermute only.
A program may use at most 128 MiB of HBM per device.

```python
import math
import jax
import jax.numpy as jnp
import numpy as np
from jax import lax

D = 2048
FF = 5632
EXPERTS = 4
TOP = 2
TOK_DEV = 192
CAP = 128
TOKENS = 768
COPIES = 1


def strengthened(values, own_key, source, target, blocks, factor):
    def block_of(axis_at):
        return (jnp.arange(values.shape[axis_at]) // (values.shape[axis_at] // blocks)).reshape((-1,) + (1,) * (values.ndim - 1 - axis_at))

    one_side = jax.random.permutation(own_key, blocks)[block_of(target)]
    other_side = (block_of(target) + blocks // 2) % blocks
    return jnp.where((block_of(source) == one_side) | (block_of(source) == other_side), factor * values, values)


def levels(key, extent, pieces, least, largest):
    loudness = 1.0
    for dim, blocks in pieces:
        draws = jax.random.uniform(jax.random.fold_in(jax.random.fold_in(key, 6), dim), (blocks,), jnp.float32, least / len(pieces), largest / len(pieces))
        loudness = loudness * jnp.repeat(jnp.exp(draws), extent[dim] // blocks).reshape((-1,) + (1,) * (len(extent) - 1 - dim))
    return loudness


def routed_block(own_key, own, number, rows, count, top, bound, lean):
    order = jax.random.permutation(own_key, count)
    packed, usual = portions_of(count, rows * top, bound, lean, True), portions_of(count, rows * top, bound, lean, False)
    places = jnp.arange(count)

    def named(lengths, turn):
        used = int((lengths > 0).sum())
        fixed = max(1, used // 4)
        moved = fixed + (places - fixed + turn * (used - fixed)) % max(1, count - fixed)
        return jnp.zeros((count,), jnp.int32).at[order[jnp.where(places < fixed, places, moved)]].set(jnp.asarray(lengths, jnp.int32))

    lengths = jnp.where(number % 4 == 0, named(packed, number // 4), named(usual, number - number // 4 - 1))
    mixed = jax.random.permutation(jax.random.fold_in(own, 3), count)
    giver, sink = mixed[0:count // 2 * 2:2], mixed[1:count // 2 * 2:2]
    slack = jnp.minimum(lengths[giver] - 1, bound - lengths[sink]) // 2
    slack = jnp.where((giver == order[0]) | (sink == order[0]) | (lengths[sink] == 0), 0, jnp.maximum(slack, 0))
    moved = jax.random.randint(jax.random.fold_in(own, 4), (count // 2,), 0, 1 << 20) % (slack + 1)
    lengths = lengths.at[giver].add(-moved).at[sink].add(moved)
    items = jnp.searchsorted(jnp.cumsum(lengths), jnp.arange(rows * top), side="right").astype(jnp.int32)
    table = items.reshape(top, rows).T
    table = table[jax.random.permutation(jax.random.fold_in(own, 1), rows)]
    turn = jax.random.randint(jax.random.fold_in(own, 2), (rows, 1), 0, top)
    return jnp.take_along_axis(table, (jnp.arange(top)[None, :] + turn) % top, axis=1)


def portions_of(amount, total, limit, slope, full):
    weights = [(1 << 20) // math.isqrt(grade ** slope) + 1 for grade in range(1, amount + 1)]
    largest = limit if full else min(limit, max(-(-total // amount), total * weights[0] // sum(weights)))
    least = 1 if total - largest >= amount - 1 else 0
    holding, rest = [largest] + [least] * (amount - 1), total - largest - least * (amount - 1)
    while rest > 0:
        movable = [i for i in range(1, amount) if holding[i] < largest] or [i for i in range(1, amount) if holding[i] < limit]
        whole, left = sum([weights[i] for i in movable]), rest
        for i in movable:
            extra = min(limit - holding[i], max(1, left * weights[i] // whole), rest)
            holding[i] = holding[i] + extra
            rest = rest - extra
    return np.array(holding)


def gaussian(key, shape, width, limit, pieces=(), kind=jnp.bfloat16):
    values = jax.random.normal(key, shape, jnp.float32) * width
    if len(pieces) > 0:
        values = levels(key, shape, pieces, -0.22, 0.18) * values
    return jnp.clip(values, min=-limit, max=limit).astype(kind)


def gaussian_with(stream_key, dims, spread, most, split, heavy, held_as=jnp.bfloat16):
    drawn = spread * jax.random.normal(stream_key, dims, jnp.float32)
    if split:
        drawn = drawn * levels(stream_key, dims, split, -0.22, 0.18)
    return jnp.clip(strengthened(drawn, jax.random.fold_in(stream_key, 3), *heavy), -most, most).astype(held_as)


def setup_inputs(seed: int = 0, part: int = 0) -> dict:
    streams_of = jax.random.split(jax.random.key(seed), 8)
    part_splits = jax.random.split(jax.random.fold_in(streams_of[7], part), 8)
    tokens = gaussian(part_splits[0], (TOKENS, D), 1.0, 6.0, ((0, 4),))
    routes_keys = jax.random.split(jax.random.fold_in(part_splits[1], 1), TOKENS // TOK_DEV)
    routes_turns = jax.random.permutation(jax.random.fold_in(part_splits[1], 3), TOKENS // TOK_DEV)
    routes = jax.vmap(lambda own, number: routed_block(jax.random.fold_in(part_splits[1], 2), own, number, TOK_DEV, EXPERTS, TOP, CAP, 1))(routes_keys, routes_turns).reshape((TOKENS, TOP))
    route_weight = jnp.clip(0.2 + 0.8 * jax.random.uniform(part_splits[2], (TOKENS, TOP), jnp.float32) ** levels(part_splits[2], (TOKENS, TOP), ((0, 4),), -0.2, 0.2), 0.2, 1.0)
    norm_gain = jnp.clip(1.0 + 0.18 * jax.random.normal(streams_of[3], (D,), jnp.float32), 0.1, 1.9)
    gate_train = gaussian(streams_of[4], (EXPERTS, D, FF), D ** -0.5, 0.125, ((0, 4), (1, 4)), jnp.float32)
    up_train = gaussian(streams_of[5], (EXPERTS, D, FF), D ** -0.5, 0.125, ((0, 4), (1, 4)), jnp.float32)
    down_train = gaussian_with(streams_of[6], (EXPERTS, FF, D), FF ** -0.5, 0.109375, ((0, 4), (2, 4)), (1, 2, 4, 2.0), jnp.float32)
    return {"tokens": tokens, "routes": routes, "route_weight": route_weight, "norm_gain": norm_gain, "gate_train": gate_train, "up_train": up_train, "down_train": down_train}


def reference(tokens, routes, route_weight, norm_gain, gate_train, up_train, down_train):
    gain_column = norm_gain[None, :, None]
    gate_low = (gate_train * gain_column).astype(jnp.bfloat16)
    up_low = (up_train * gain_column).astype(jnp.bfloat16)
    down_low = down_train.astype(jnp.bfloat16)
    tok_float = tokens.astype(jnp.float32)
    normed = (tok_float * lax.rsqrt(lax.optimization_barrier(jnp.mean(tok_float * tok_float, axis=-1, keepdims=True)) + 1e-06)).astype(jnp.bfloat16)
    normed_wide = normed.astype(jnp.float32)

    def expert(triple):
        gate_one, up_one, down_one = triple
        gated = jnp.dot(normed_wide, gate_one.astype(jnp.float32), preferred_element_type=jnp.float32)
        lifted = jnp.dot(normed_wide, up_one.astype(jnp.float32), preferred_element_type=jnp.float32)
        hidden = (jax.nn.silu(gated) * lifted).astype(jnp.bfloat16)
        return jnp.dot(hidden.astype(jnp.float32), down_one.astype(jnp.float32), preferred_element_type=jnp.float32).astype(jnp.bfloat16)
    outputs = lax.map(expert, (gate_low, up_low, down_low))
    row_index = jnp.arange(tokens.shape[0], dtype=jnp.int32)
    first = outputs[routes[:, 0], row_index].astype(jnp.float32)
    second = outputs[routes[:, 1], row_index].astype(jnp.float32)
    mixed = route_weight[:, 0:1] * first + route_weight[:, 1:2] * second
    gate_serve = jnp.tile(gate_low, (1, 1, COPIES))
    up_serve = jnp.tile(up_low, (1, 1, COPIES))
    down_serve = jnp.tile(down_low, (1, COPIES, 1))
    return (gate_serve, up_serve, down_serve, mixed.astype(jnp.bfloat16))
```

```python
import jax
import jax.numpy as jnp
from jax import lax
from jax.sharding import PartitionSpec as P

EXPERTS = 4
CAP = 128
BF = jnp.bfloat16


def slots_of(routes):
    chosen = routes.reshape(-1)
    hot = (chosen[:, None] == jnp.arange(EXPERTS, dtype=jnp.int32)[None, :]).astype(jnp.int32)
    before = jnp.cumsum(hot, axis=0) - hot
    rank = jnp.sum(before * hot, axis=1)
    return (chosen * CAP + rank).reshape(routes.shape)


def norm_rows(tokens):
    wide = tokens.astype(jnp.float32)
    scale = lax.rsqrt(jnp.mean(wide * wide, axis=-1, keepdims=True) + 1e-06)
    return (wide * scale).astype(BF)


def dispatch(normed, slot_index):
    slot_range = jnp.arange(EXPERTS * CAP, dtype=jnp.int32)
    pick = jnp.any(slot_range[:, None, None] == slot_index[None, :, :], axis=-1).astype(BF)
    outgoing = jnp.dot(pick, normed, preferred_element_type=jnp.float32).astype(BF)
    outgoing = outgoing.reshape(EXPERTS, CAP, normed.shape[1])
    arrived = lax.all_to_all(outgoing, "tp", split_axis=0, concat_axis=0, tiled=True)
    return arrived.reshape(EXPERTS * CAP, normed.shape[1])


def come_home(partial_out, slot_index, route_weight):
    cols = partial_out.shape[1]
    back = lax.all_to_all(
        partial_out.astype(BF).reshape(EXPERTS, CAP, cols), "tp", split_axis=0, concat_axis=0, tiled=True
    ).reshape(EXPERTS * CAP, cols)
    slot_range = jnp.arange(EXPERTS * CAP, dtype=jnp.int32)
    total = None
    for i in range(slot_index.shape[1]):
        hot = (slot_range[None, :] == slot_index[:, i : i + 1]).astype(BF)
        rows = jnp.dot(hot, back, preferred_element_type=jnp.float32)
        term = route_weight[:, i : i + 1] * rows
        total = term if total is None else total + term
    return total


def halved(tokens, routes, route_weight, norm_gain, gate_train, up_train, down_train):
    n = lax.axis_size("fs")
    me = lax.axis_index("fs")
    mine = lax.axis_index("grp")
    dl = gate_train.shape[1]
    ff = gate_train.shape[2]
    hid = ff // n
    half = dl // 2
    D = dl * n
    swap = [(0, 1), (1, 0)]

    def shift(x, k):
        return lax.ppermute(x, "fs", [(i, (i + k) % n) for i in range(n)])

    gain = norm_gain[:, None]

    def wide_piece(src, row0, rows, col0, cols):
        part = lax.dynamic_slice(src[0], (row0, col0), (rows, cols))
        return (part * lax.dynamic_slice(gain, (row0, 0), (rows, 1))).astype(BF)

    def down_piece(row0, rows, col0, cols):
        return lax.dynamic_slice(down_train[0], (row0, col0), (rows, cols)).astype(BF)

    order = [1, n - 1] + list(range(2, n - 1))

    slot_index = slots_of(routes)
    my_rows = dispatch(norm_rows(tokens), slot_index)

    def spread(src):
        out = jnp.zeros((D, hid), BF)
        out = lax.dynamic_update_slice(out, wide_piece(src, 0, dl, me * hid, hid), (me * dl, 0))
        for k in order:
            sent = wide_piece(src, mine * half, half, ((me + k) % n) * hid, hid)
            got = shift(sent, k)
            other = lax.ppermute(got, "grp", swap)
            s = (me - k) % n
            out = lax.dynamic_update_slice(out, got, (s * dl + mine * half, 0))
            out = lax.dynamic_update_slice(out, other, (s * dl + (1 - mine) * half, 0))
        return out

    gate_new = spread(gate_train)
    up_new = spread(up_train)
    gated = jnp.dot(my_rows, gate_new, preferred_element_type=jnp.float32)
    lifted = jnp.dot(my_rows, up_new, preferred_element_type=jnp.float32)
    hidden = (jax.nn.silu(gated) * lifted).astype(BF)

    def home(block):
        part = jnp.dot(hidden, block, preferred_element_type=jnp.float32)
        return come_home(part, slot_index, route_weight)

    own = down_piece(me * hid, hid, 0, dl)
    down_new = lax.dynamic_update_slice(jnp.zeros((hid, D), BF), own, (0, me * dl))
    mixed = home(own)
    for k in order:
        sent = down_piece(((me + k) % n) * hid, hid, mine * half, half)
        got = shift(sent, k)
        other = lax.ppermute(got, "grp", swap)
        s = (me - k) % n
        block = jnp.zeros((hid, dl), BF)
        block = lax.dynamic_update_slice(block, got, (0, mine * half))
        block = lax.dynamic_update_slice(block, other, (0, (1 - mine) * half))
        down_new = lax.dynamic_update_slice(down_new, block, (0, s * dl))
        part = home(block).astype(BF)
        mixed = mixed + shift(part, n - k).astype(jnp.float32)
    return (gate_new[None], up_new[None], down_new[None], mixed.astype(BF))


def exchanged(tokens, routes, route_weight, norm_gain, gate_train, up_train, down_train):
    n = lax.axis_size("fs")
    pieces = min(n, 32)
    copies = n // pieces
    gain = norm_gain[:, None]
    gate_low = jnp.tile((gate_train[0] * gain).astype(BF), (1, copies))
    up_low = jnp.tile((up_train[0] * gain).astype(BF), (1, copies))
    down_low = jnp.tile(down_train[0].astype(BF), (copies, 1))
    gate_new = lax.all_to_all(gate_low, "fs", split_axis=1, concat_axis=0, tiled=True)
    up_new = lax.all_to_all(up_low, "fs", split_axis=1, concat_axis=0, tiled=True)
    down_new = lax.all_to_all(down_low, "fs", split_axis=0, concat_axis=1, tiled=True)
    slot_index = slots_of(routes)
    arrived = dispatch(norm_rows(tokens), slot_index)
    count = EXPERTS * CAP // copies
    copy_index = lax.axis_index("fs") // pieces
    my_rows = lax.dynamic_slice_in_dim(arrived, copy_index * count, count, 0)
    gated = jnp.dot(my_rows, gate_new, preferred_element_type=jnp.float32)
    lifted = jnp.dot(my_rows, up_new, preferred_element_type=jnp.float32)
    hidden = (jax.nn.silu(gated) * lifted).astype(BF)
    partial_out = jnp.dot(hidden, down_new, preferred_element_type=jnp.float32)
    placed = jnp.zeros((EXPERTS * CAP, partial_out.shape[1]), jnp.float32)
    placed = lax.dynamic_update_slice_in_dim(placed, partial_out, copy_index * count, 0)
    expert_out = lax.psum_scatter(placed, "fs", scatter_dimension=1, tiled=True)
    mixed = come_home(expert_out, slot_index, route_weight)
    return (gate_new[None], up_new[None], down_new[None], mixed.astype(BF))


def solution(mesh):
    in_specs = (
        P(("grp", "tp"), None),
        P(("grp", "tp"), None),
        P(("grp", "tp"), None),
        P("fs"),
        P("tp", "fs", None),
        P("tp", "fs", None),
        P("tp", None, "fs"),
    )
    out_specs = (
        P(("grp", "tp"), None, "fs"),
        P(("grp", "tp"), None, "fs"),
        P(("grp", "tp"), "fs", None),
        P(("grp", "tp"), "fs"),
    )
    few = mesh.shape["fs"] <= 8 and mesh.shape["grp"] == 2
    body = halved if few else exchanged
    return jax.shard_map(body, mesh=mesh, in_specs=in_specs, out_specs=out_specs, check_vma=False)
```
